512 devices in a mesh: sp: 32 (over z, x), tp: 16 (over y, core).
Axes of the slice: x: 4, y: 8, z: 8, core: 2. Of those that a mesh axis runs over, the one named last changes fastest.
Arguments:
- residual: bfloat16 [8192, 2048], P('sp', 'tp'), may hold values from -6 to 6
- queries: bfloat16 [8192, 1024], P('sp', 'tp'), may hold values from -5.5 to 5.5
- keys: bfloat16 [8192, 128], P('sp'), may hold values from -5.5 to 5.5
- values: bfloat16 [8192, 128], P('sp'), may hold values from -6 to 6
- documents: int32 [8192], P('sp'), may hold values from 0 to 15, never falling along the last dimension, each value on 1 to 1024 neighbouring positions
- sinks: float32 [16], P('tp'), may hold values from 1 to 6
- head_gain: float32 [1024], replicated, may hold values from 0.1 to 1.9
- out_weight: bfloat16 [1024, 2048], P(None, 'tp'), may hold values from -0.1875 to 0.1875
- norm_gain: float32 [2048], P('tp'), may hold values from 0.1 to 1.9
- norm_shift: float32 [2048], P('tp'), may hold values from -3 to 3
- routes: int32 [8192, 2], P('sp'), may hold values from 0 to 31, all different within a row; in each aligned block of 256 rows (0 to 255, 256 to 511, ...) at most 24 rows name the same one
- route_logits: float32 [8192, 2], P('sp'), may hold values from -150 to 150
- gate_weight: bfloat16 [32, 2048, 6144], P('sp', None, 'tp'), may hold values from -0.125 to 0.125
- up_weight: bfloat16 [32, 2048, 6144], P('sp', None, 'tp'), may hold values from -0.125 to 0.125
- down_weight: bfloat16 [32, 6144, 2048], P('sp', 'tp'), may hold values from -0.15625 to 0.15625
- final_gain: float32 [2048], P('tp'), may hold values from 0.1 to 1.9
- final_shift: float32 [2048], P('tp'), may hold values from -3 to 3
Outputs:
- layer_out: bfloat16 [8192, 2048], P('sp', 'tp')
The draws below stay inside these ranges and needn't reach their ends.
Inputs may be any that keep to these rules, and one draw needn't show every extreme that they name: `documents`: document numbers never fall along the sequence; each document has at least one position and at most 1024, and some document has exactly 1024. `routes`: each row names 2 different experts. In each aligned block of 256 rows (the rows of one index of sp) no expert is named by more than 24 rows, a bound that some block reaches.
All inputs are finite; a program needn't handle non-finite values.
Results may differ from the reference program's by a relative error of at most 0.014.
Values may be sent and summed in bfloat16 or wider, within the bound.
A program may use at most 128 MiB of HBM per device.

```python
import math
import jax
import jax.numpy as jnp
import numpy as np
from jax import lax

D = 2048
QUERY_HEADS = 16
KEY_VALUE_HEADS = 2
HEAD_SIZE = 64
FF = 6144
WINDOW_SIZE = 128
TOP = 2
TOK_SP = 256
PACKED_TOKENS = 8192
EXPERTS = 32
CAP = 24
DOCS = 16
DOC_MOST = 1024
N_SP = 32
N_TP = 16


def drawn_sample(key, salt, head_list):
    base = jax.random.truncated_normal(jax.random.fold_in(key, salt), -5.0, 5.0, (PACKED_TOKENS, head_list, HEAD_SIZE), jnp.float32)
    return base.reshape(PACKED_TOKENS, head_list * HEAD_SIZE).astype(jnp.bfloat16)


def draw_queries(key, part):
    return drawn_sample(key, 11, QUERY_HEADS)


def draw_keys(key, part):
    return drawn_sample(key, 13, KEY_VALUE_HEADS)


def draw_route_logits(key, part):
    logits = 1.5 * jax.random.truncated_normal(jax.random.fold_in(key, 17), -4.0, 4.0, (PACKED_TOKENS, TOP), jnp.float32)
    return logits


def block_scale(stream_key, extent, pieces, smallest, largest):
    level = 1.0
    for position, blocks in pieces:
        draws = jax.random.uniform(jax.random.fold_in(jax.random.fold_in(stream_key, 6), position), (blocks,), jnp.float32, smallest / len(pieces), largest / len(pieces))
        level = level * jnp.repeat(jnp.exp(draws), extent[position] // blocks).reshape((-1,) + (1,) * (len(extent) - 1 - position))
    return level


def profile(number_of, total, bound, lean):
    weights = [(1 << 20) // math.isqrt(standing ** lean) + 1 for standing in range(2, number_of + 1)]
    spare, counts = total - bound - (number_of - 1), [1] * (number_of - 1)
    while spare > 0:
        movable = [i for i in range(number_of - 1) if counts[i] < bound]
        mass, left = sum([weights[i] for i in movable]), spare
        for i in movable:
            addition = min(bound - counts[i], max(1, left * weights[i] // mass), spare)
            counts[i] = counts[i] + addition
            spare = spare - addition
    return np.array([bound] + counts)


def uneven_parts(stream_key, number_of, total, bound, skew):
    if number_of == 2:
        one = jax.random.randint(stream_key, (), max(1, total - bound), min(bound, total - 1) + 1)
        return jnp.stack([one, total - one])
    tallies = jnp.asarray(profile(number_of, total, bound, skew), jnp.int32)
    pairs = (number_of - 1) // 2
    giver, receiver = tallies[1:1 + 2 * pairs:2], tallies[2:2 + 2 * pairs:2]
    margin = jnp.minimum(giver - 1, bound - receiver)
    moved = jax.random.randint(jax.random.fold_in(stream_key, 1), (pairs,), 0, 1 << 20) % (margin + 1)
    tallies = tallies.at[1:1 + 2 * pairs:2].set(giver - moved).at[2:2 + 2 * pairs:2].set(receiver + moved)
    return tallies[jax.random.permutation(jax.random.fold_in(stream_key, 2), number_of)]


def deal_out(key, own, number, rows, number_of, top, reach, lean):
    order = jax.random.permutation(key, number_of)
    crowded, usual = shares(number_of, rows * top, reach, lean, True), shares(number_of, rows * top, reach, lean, False)
    places = jnp.arange(number_of)

    def named(lengths, turn):
        used = int((lengths > 0).sum())
        fixed = max(1, used // 4)
        passed = fixed + (places - fixed + turn * (used - fixed)) % max(1, number_of - fixed)
        return jnp.zeros((number_of,), jnp.int32).at[order[jnp.where(places < fixed, places, passed)]].set(jnp.asarray(lengths, jnp.int32))

    lengths = jnp.where(number % 4 == 0, named(crowded, number // 4), named(usual, number - number // 4 - 1))
    mixed = jax.random.permutation(jax.random.fold_in(own, 3), number_of)
    donor, receiver = mixed[0:number_of // 2 * 2:2], mixed[1:number_of // 2 * 2:2]
    room = jnp.minimum(lengths[donor] - 1, reach - lengths[receiver]) // 2
    room = jnp.where((donor == order[0]) | (receiver == order[0]) | (lengths[receiver] == 0), 0, jnp.maximum(room, 0))
    passed = jax.random.randint(jax.random.fold_in(own, 4), (number_of // 2,), 0, 1 << 20) % (room + 1)
    lengths = lengths.at[donor].add(-passed).at[receiver].add(passed)
    members = jnp.searchsorted(jnp.cumsum(lengths), jnp.arange(rows * top), side="right").astype(jnp.int32)
    table = members.reshape(top, rows).T
    table = table[jax.random.permutation(jax.random.fold_in(own, 1), rows)]
    turn = jax.random.randint(jax.random.fold_in(own, 2), (rows, 1), 0, top)
    return jnp.take_along_axis(table, (jnp.arange(top)[None, :] + turn) % top, axis=1)


def shares(count, total, most, skew, full):
    weights = [(1 << 20) // math.isqrt(grade ** skew) + 1 for grade in range(1, count + 1)]
    largest = most if full else min(most, max(-(-total // count), total * weights[0] // sum(weights)))
    least = 1 if total - largest >= count - 1 else 0
    given, spare = [largest] + [least] * (count - 1), total - largest - least * (count - 1)
    while spare > 0:
        movable = [i for i in range(1, count) if given[i] < largest] or [i for i in range(1, count) if given[i] < most]
        whole, left = sum([weights[i] for i in movable]), spare
        for i in movable:
            extra = min(most - given[i], max(1, left * weights[i] // whole), spare)
            given[i] = given[i] + extra
            spare = spare - extra
    return np.array(given)


def scatter_about(stream_key, extent, width, bound, split=(), held_as=jnp.bfloat16):
    entries = width * jax.random.normal(stream_key, extent, jnp.float32)
    if split:
        entries = entries * block_scale(stream_key, extent, split, -0.22, 0.18)
    return jnp.clip(entries, -bound, bound).astype(held_as)


def setup_inputs(seed: int = 0) -> dict:
    streams_of = jax.random.split(jax.random.key(seed), 18)
    residual = scatter_about(streams_of[0], (PACKED_TOKENS, D), 1.0, 6.0, ((0, 32), (1, 16)))
    queries = draw_queries(jax.random.fold_in(streams_of[17], 71), 0)
    keys = draw_keys(jax.random.fold_in(streams_of[17], 71), 0)
    values = scatter_about(streams_of[3], (PACKED_TOKENS, KEY_VALUE_HEADS * HEAD_SIZE), 1.0, 6.0, ((0, 32),))
    documents = jnp.searchsorted(jnp.cumsum(uneven_parts(streams_of[4], DOCS, PACKED_TOKENS, DOC_MOST, 1)), jnp.arange(PACKED_TOKENS), side="right").astype(jnp.int32)
    sinks = jnp.clip(1.0 + 5.0 * jax.random.uniform(streams_of[5], (QUERY_HEADS,), jnp.float32) ** block_scale(streams_of[5], (QUERY_HEADS,), ((0, 16),), -0.2, 0.2), 1.0, 6.0)
    head_gain = jnp.clip(1.0 + 0.18 * jax.random.normal(streams_of[6], (QUERY_HEADS * HEAD_SIZE,), jnp.float32), 0.1, 1.9)
    out_weight = scatter_about(streams_of[7], (QUERY_HEADS * HEAD_SIZE, D), (QUERY_HEADS * HEAD_SIZE) ** -0.5, 0.1875, ((1, 16),))
    norm_gain = jnp.clip(1.0 + 0.18 * jax.random.normal(streams_of[8], (D,), jnp.float32), 0.1, 1.9)
    norm_shift = scatter_about(streams_of[9], (D,), 0.5, 3.0, ((0, 16),), jnp.float32)
    routes_keys = jax.random.split(jax.random.fold_in(streams_of[10], 1), PACKED_TOKENS // TOK_SP)
    routes_turns = jax.random.permutation(jax.random.fold_in(streams_of[10], 3), PACKED_TOKENS // TOK_SP)
    routes = jax.vmap(lambda own, number: deal_out(jax.random.fold_in(streams_of[10], 2), own, number, TOK_SP, EXPERTS, TOP, CAP, 1))(routes_keys, routes_turns).reshape((PACKED_TOKENS, TOP))
    route_logits = draw_route_logits(jax.random.fold_in(streams_of[17], 71), 0)
    gate_weight = scatter_about(streams_of[12], (EXPERTS, D, FF), D ** -0.5, 0.125, ((0, 32), (2, 16)))
    up_weight = scatter_about(streams_of[13], (EXPERTS, D, FF), D ** -0.5, 0.125, ((0, 32), (2, 16)))
    down_weight = scatter_about(streams_of[14], (EXPERTS, FF, D), (FF // 4) ** -0.5, 0.15625, ((0, 32), (1, 16)))
    final_gain = jnp.clip(1.0 + 0.18 * jax.random.normal(streams_of[15], (D,), jnp.float32), 0.1, 1.9)
    final_shift = scatter_about(streams_of[16], (D,), 0.5, 3.0, ((0, 16),), jnp.float32)
    return {"residual": residual, "queries": queries, "keys": keys, "values": values, "documents": documents, "sinks": sinks, "head_gain": head_gain, "out_weight": out_weight, "norm_gain": norm_gain, "norm_shift": norm_shift, "routes": routes, "route_logits": route_logits, "gate_weight": gate_weight, "up_weight": up_weight, "down_weight": down_weight, "final_gain": final_gain, "final_shift": final_shift}


DEEP_ALPHA = 8.0 ** 0.25
NORM_EPS = 1e-05

def layer_norm(total, gain, shift):
    center = lax.optimization_barrier(jnp.sum(total, axis=-1, keepdims=True)) / D
    spread = lax.optimization_barrier(jnp.sum(total * total, axis=-1, keepdims=True)) / D - center * center
    return (total - center) * lax.rsqrt(spread + NORM_EPS) * gain + shift

def window_attention(queries, keys, values, documents, sinks):
    query_group = QUERY_HEADS // KEY_VALUE_HEADS
    padded_key_rows = jnp.concatenate([jnp.zeros((WINDOW_SIZE, KEY_VALUE_HEADS * HEAD_SIZE), jnp.bfloat16), keys], axis=0)
    padded_value_rows = jnp.concatenate([jnp.zeros((WINDOW_SIZE, KEY_VALUE_HEADS * HEAD_SIZE), jnp.bfloat16), values], axis=0)
    pad_docs = jnp.concatenate([jnp.full((WINDOW_SIZE,), -1, jnp.int32), documents.astype(jnp.int32)], axis=0)
    query_blocks = queries.reshape(PACKED_TOKENS // WINDOW_SIZE, WINDOW_SIZE, QUERY_HEADS, HEAD_SIZE)

    def one_block(inputs):
        query_block, index = inputs
        window_begin = (index * WINDOW_SIZE).astype(jnp.int32)
        key_tile_block = lax.dynamic_slice_in_dim(padded_key_rows, window_begin, 2 * WINDOW_SIZE, 0).reshape(2 * WINDOW_SIZE, KEY_VALUE_HEADS, HEAD_SIZE)
        value_tile_block = lax.dynamic_slice_in_dim(padded_value_rows, window_begin, 2 * WINDOW_SIZE, 0).reshape(2 * WINDOW_SIZE, KEY_VALUE_HEADS, HEAD_SIZE)
        key_docs = lax.dynamic_slice_in_dim(pad_docs, window_begin, 2 * WINDOW_SIZE, 0)
        query_docs = lax.dynamic_slice_in_dim(documents.astype(jnp.int32), window_begin, WINDOW_SIZE, 0)
        key_wide = jnp.repeat(key_tile_block, query_group, axis=1)
        value_wide = jnp.repeat(value_tile_block, query_group, axis=1)
        scores = jnp.einsum('qhd,khd->hqk', query_block.astype(jnp.float32), key_wide.astype(jnp.float32)) * HEAD_SIZE ** (-0.5)
        query_pos = window_begin + jnp.arange(WINDOW_SIZE, dtype=jnp.int32)
        key_pos = window_begin - WINDOW_SIZE + jnp.arange(2 * WINDOW_SIZE, dtype=jnp.int32)
        distance = query_pos[:, None] - key_pos[None, :]
        allowed = (distance >= 0) & (distance < WINDOW_SIZE) & (key_pos[None, :] >= 0) & (query_docs[:, None] == key_docs[None, :])
        scores = jnp.where(allowed[None], scores, -jnp.inf)
        sink_col = sinks.astype(jnp.float32)[:, None]
        top = jnp.maximum(lax.optimization_barrier(jnp.max(scores, axis=-1)), sink_col)
        expd = jnp.exp(scores - top[..., None])
        probs = (expd / (lax.optimization_barrier(jnp.sum(expd, axis=-1)) + jnp.exp(sink_col - top))[..., None]).astype(jnp.bfloat16)
        result = jnp.einsum('hqk,khd->qhd', probs.astype(jnp.float32), value_wide.astype(jnp.float32))
        return result.astype(jnp.bfloat16)
    blocks = lax.map(one_block, (query_blocks, jnp.arange(PACKED_TOKENS // WINDOW_SIZE, dtype=jnp.int32)))
    return blocks.reshape(PACKED_TOKENS, QUERY_HEADS * HEAD_SIZE)

def reference(residual, queries, keys, values, documents, sinks, head_gain, out_weight, norm_gain, norm_shift, routes, route_logits, gate_weight, up_weight, down_weight, final_gain, final_shift):
    attended = window_attention(queries, keys, values, documents, sinks).astype(jnp.float32)
    scaled = (attended * lax.rsqrt(lax.optimization_barrier(jnp.mean(attended * attended, axis=-1, keepdims=True)) + NORM_EPS) * head_gain).astype(jnp.bfloat16)
    mix = jnp.dot(scaled, out_weight, preferred_element_type=jnp.float32)
    first = DEEP_ALPHA * residual.astype(jnp.float32) + mix
    hidden = layer_norm(first, norm_gain, norm_shift)
    hidden_rows = hidden.astype(jnp.bfloat16)
    flat = routes.astype(jnp.int32).reshape(N_SP, TOK_SP * TOP)
    onehot = (flat[..., None] == jnp.arange(EXPERTS, dtype=jnp.int32)).astype(jnp.int32)
    rank = lax.optimization_barrier(jnp.sum(jnp.cumsum(onehot, axis=1) * onehot, axis=-1)) - 1
    source = jnp.arange(N_SP, dtype=jnp.int32)[:, None]
    place = ((flat * N_SP + source) * CAP + rank).astype(jnp.int32)
    owner = source * TOK_SP + jnp.arange(TOK_SP * TOP, dtype=jnp.int32)[None, :] // TOP
    table = jnp.full((EXPERTS * N_SP * CAP,), PACKED_TOKENS, jnp.int32).at[place.reshape(-1)].set(owner.reshape(-1).astype(jnp.int32))
    padded = jnp.concatenate([hidden_rows, jnp.zeros((1, D), jnp.bfloat16)], axis=0)

    def one_expert(inputs):
        index_rows, gate_w, up_w, down_w = inputs
        picked_rows = padded[index_rows]
        gate = jnp.dot(picked_rows, gate_w, preferred_element_type=jnp.float32)
        up_val = jnp.dot(picked_rows, up_w, preferred_element_type=jnp.float32)
        middle = (jax.nn.silu(gate) * up_val).astype(jnp.bfloat16)
        blocks = jnp.einsum('rjf,jfd->rjd', middle.reshape(-1, N_TP, FF // N_TP).astype(jnp.float32), down_w.reshape(N_TP, FF // N_TP, D).astype(jnp.float32))
        blocks = blocks.astype(jnp.bfloat16).astype(jnp.float32)
        return lax.optimization_barrier(jnp.sum(blocks, axis=1)).astype(jnp.bfloat16)
    outputs = lax.map(one_expert, (table.reshape(EXPERTS, N_SP * CAP), gate_weight, up_weight, down_weight))
    expert_out = outputs.reshape(EXPERTS * N_SP * CAP, D)[place.reshape(-1)].reshape(PACKED_TOKENS, TOP, D).astype(jnp.float32)
    share = jax.nn.softmax(route_logits.astype(jnp.float32), axis=-1)
    moe = lax.optimization_barrier(jnp.sum(share[:, :, None] * expert_out, axis=1))
    second = DEEP_ALPHA * hidden + moe
    return layer_norm(second, final_gain, final_shift).astype(jnp.bfloat16)
```

```python
import jax
import jax.numpy as jnp
from jax import lax
from jax.experimental import pallas as pl
from jax.experimental.pallas import tpu as pltpu
from jax.sharding import PartitionSpec as P

D = 2048
HEAD = 64
WINDOW = 128
TOK = 256
CAP = 24
SP = 32
TP = 16
NY = 8
COLS = D // TP
ROWS = SP * CAP
HALF = ROWS // 2
FFB = 384
ALPHA = 8.0**0.25
EPS = 1e-05
MESH = pl.DeviceIdType.MESH
BF = jnp.bfloat16
F32 = jnp.float32

RIGHT = [(0, 0), (0, 1), (1, 0), (1, 1), (2, 0), (2, 1), (3, 0)]
LEFT = [(0, 1), (0, 0), (1, 1), (1, 0), (2, 1), (2, 0), (3, 1)]
DESTS = [4, 3, 5, 2, 6, 1, 7, 0]
SUM_RIGHT = [(0, 0), (1, 1), (1, 0), (3, 1), (3, 0), (5, 1), (5, 0)]
SUM_LEFT = [(0, 1), (2, 0), (2, 1), (4, 0), (4, 1), (6, 0), (6, 1)]


def dot(a, b):
    return lax.dot_general(a, b, (((1,), (0,)), ((), ())), preferred_element_type=F32)


def dot_nt(a, b):
    return lax.dot_general(a, b, (((1,), (1,)), ((), ())), preferred_element_type=F32)


def column(row):
    return jnp.transpose(jnp.broadcast_to(row, (128, 128)))


def twice(a):
    return jnp.concatenate([a, a], axis=1)


def kernel(
    residual, queries, keys, values, docs, sinks, head_gain, out_weight, norm_gain, norm_shift,
    routes, logits, final_gain, final_shift, gate_hbm, up_hbm, down_hbm,
    out,
    wgu, wd, tail_k, tail_v, tail_d, wot, res, vt, select, mix_hi, mix_lo,
    att, stat1, stat2, hid, going, came, grid, acc, mid, mine, sib_out, sib_in,
    right_out, right_in, left_out, left_in, back_out, back_in,
    w_sem, tail_sem, a_send, a_recv, as_send, as_recv, s_send, s_recv, s2_send, s2_recv,
    d_send, d_recv, gr_send, gr_recv, gl_send, gl_recv, gs_send, gs_recv,
    rs_send, rs_recv, rr_send, rr_recv, rl_send, rl_recv, b_send, b_recv, own_sem,
):
    sp = lax.axis_index("sp")
    tp = lax.axis_index("tp")
    y = lax.div(tp, 2)
    c = lax.rem(tp, 2)
    sibling = {"tp": y * 2 + 1 - c}

    def chip(distance):
        return lax.rem(y + distance, NY)

    def on_y(distance):
        return {"tp": chip(distance) * 2 + c}

    def send(src, dst, send_sem, recv_sem, device):
        pltpu.make_async_remote_copy(
            src_ref=src, dst_ref=dst, send_sem=send_sem, recv_sem=recv_sem,
            device_id=device, device_id_type=MESH,
        ).start()

    def arrived(dst, send_sem, recv_sem, device):
        pltpu.make_async_remote_copy(
            src_ref=dst, dst_ref=dst, send_sem=send_sem, recv_sem=recv_sem,
            device_id=device, device_id_type=MESH,
        ).wait_recv()

    def left_here(src, send_sem, recv_sem, device):
        pltpu.make_async_remote_copy(
            src_ref=src, dst_ref=src, send_sem=send_sem, recv_sem=recv_sem,
            device_id=device, device_id_type=MESH,
        ).wait_send()

    w_copies = [
        pltpu.make_async_copy(gate_hbm.at[0], wgu.at[:, 0:FFB], w_sem.at[0]),
        pltpu.make_async_copy(up_hbm.at[0], wgu.at[:, FFB : 2 * FFB], w_sem.at[1]),
    ]
    for d in range(NY):
        for part in range(2):
            block = 2 * d + (c if part == 0 else 1 - c)
            w_copies.append(
                pltpu.make_async_copy(
                    down_hbm.at[0, :, pl.ds(pl.multiple_of(block * 128, 128), 128)],
                    wd.at[d, :, 128 * part : 128 * part + 128],
                    w_sem.at[2 + 2 * d + part],
                )
            )
    for copy in w_copies:
        copy.start()

    barrier = pltpu.get_barrier_semaphore()

    def greet_tp(k, carry):
        pl.semaphore_signal(barrier, inc=1, device_id={"tp": lax.rem(tp + k, TP)}, device_id_type=MESH)
        return carry

    def greet_sp(k, carry):
        pl.semaphore_signal(barrier, inc=1, device_id={"sp": lax.rem(sp + k, SP)}, device_id_type=MESH)
        return carry

    lax.fori_loop(1, TP, greet_tp, 0)
    lax.fori_loop(1, SP, greet_sp, 0)

    upper = tp >= TP // 2
    vt[:, WINDOW:] = jnp.transpose(values[...].astype(F32)).astype(BF)
    qt = queries[...]
    zero_q = jnp.zeros_like(qt)
    q_wide = jnp.concatenate([jnp.where(upper, zero_q, qt), jnp.where(upper, qt, zero_q)], axis=0)
    doc_row = docs[...].astype(F32)
    sink = sinks[0, 0]

    def attend(key_rows, v_cols, key_docs, begin):
        score = dot(key_rows, q_wide[:, begin : begin + 128]) * HEAD ** (-0.5)
        ahead = (
            WINDOW
            + lax.broadcasted_iota(jnp.int32, (256, 128), 1)
            - lax.broadcasted_iota(jnp.int32, (256, 128), 0)
        )
        allowed = (ahead >= 0) & (ahead < WINDOW) & (key_docs == doc_row[:, begin : begin + 128])
        score = jnp.where(allowed, score, -1e30)
        top = jnp.maximum(jnp.max(score, axis=0, keepdims=True), sink)
        e = jnp.exp(score - top)
        total = jnp.sum(e, axis=0, keepdims=True) + jnp.exp(sink - top)
        probs = (e * (1.0 / total)).astype(BF)
        wide = dot(v_cols, probs)
        return jnp.where(upper, wide[HEAD:, :], wide[:HEAD, :]).astype(BF)

    docs0 = column(doc_row[:, 0:128])
    docs1 = column(doc_row[:, 128:256])
    att[tp, :, 128:256] = attend(keys[...], vt[:, 128:384], jnp.concatenate([docs0, docs1], axis=0), 128)

    pl.semaphore_wait(barrier, TP - 1 + SP - 1)

    after = {"sp": lax.rem(sp + 1, SP)}
    send(keys.at[128:256], tail_k, tail_sem.at[0], tail_sem.at[3], after)
    send(values.at[128:256], tail_v, tail_sem.at[1], tail_sem.at[4], after)
    send(docs.at[:, 128:256], tail_d, tail_sem.at[2], tail_sem.at[5], after)

    wot[...] = (jnp.transpose(out_weight[...].astype(F32)) * head_gain[...]).astype(BF)
    res[...] = ALPHA * jnp.transpose(residual[...].astype(F32))

    arrived(tail_k, tail_sem.at[0], tail_sem.at[3], after)
    arrived(tail_v, tail_sem.at[1], tail_sem.at[4], after)
    arrived(tail_d, tail_sem.at[2], tail_sem.at[5], after)
    vt[:, 0:WINDOW] = jnp.transpose(tail_v[...].astype(F32)).astype(BF)
    before_docs = jnp.where(sp > 0, tail_d[...].astype(F32), -1.0)
    att[tp, :, 0:128] = attend(
        jnp.concatenate([tail_k[...], keys[0:128, :]], axis=0),
        vt[:, 0:256],
        jnp.concatenate([column(before_docs), docs0], axis=0),
        0,
    )

    send(att.at[tp], att.at[tp], as_send.at[0], as_recv.at[0], sibling)
    for k in (4, 3, 5, 2, 6, 1, 7):
        send(att.at[tp], att.at[tp], a_send.at[k], a_recv.at[k], on_y(k))

    r0, r1 = routes[0:1, :], routes[1:2, :]
    experts = lax.broadcasted_iota(jnp.int32, (SP, TOK), 0)
    first_hit, second_hit = r0 == experts, r1 == experts
    named = jnp.where(first_hit | second_hit, 1.0, 0.0)
    earlier = jnp.where(
        lax.broadcasted_iota(jnp.int32, (TOK, TOK), 0) < lax.broadcasted_iota(jnp.int32, (TOK, TOK), 1), 1.0, 0.0
    ).astype(BF)
    place = jnp.where(named > 0.0, dot(named.astype(BF), earlier), -1.0)
    l0, l1 = logits[0:1, :], logits[1:2, :]
    l_top = jnp.maximum(l0, l1)
    e0, e1 = jnp.exp(l0 - l_top), jnp.exp(l1 - l_top)
    per = 1.0 / (e0 + e1)
    share = jnp.where(first_hit, e0 * per, jnp.where(second_hit, e1 * per, 0.0))
    slots = lax.broadcasted_iota(jnp.int32, (CAP, TOK), 0).astype(F32)
    for group in range(4):
        hits, weights = [], []
        for e in range(8 * group, 8 * group + 8):
            hit = place[e : e + 1, :] == slots
            hits.append(jnp.where(hit, 1.0, 0.0))
            weights.append(jnp.where(hit, share[e : e + 1, :], 0.0))
        rows = pl.ds(group * 8 * CAP, 8 * CAP)
        weight = jnp.concatenate(weights, axis=0)
        high = weight.astype(BF)
        select[rows, :] = jnp.concatenate(hits, axis=0).astype(BF)
        mix_hi[rows, :] = high
        mix_lo[rows, :] = (weight - high.astype(F32)).astype(BF)
    gain1, shift1 = twice(column(norm_gain[...])), twice(column(norm_shift[...]))

    for k in (1, 7, 2, 6, 3, 5, 4):
        block = att.at[chip(NY - k) * 2 + c]
        arrived(block, a_send.at[k], a_recv.at[k], on_y(k))
        send(block, block, as_send.at[k], as_recv.at[k], sibling)
    for k in range(NY):
        arrived(att.at[chip(NY - k) * 2 + 1 - c], as_send.at[k], as_recv.at[k], sibling)

    heads = att[...].reshape(TP * HEAD, TOK)
    wide = heads.astype(F32)
    scale = lax.rsqrt(jnp.sum(wide * wide, axis=0, keepdims=True) * (1.0 / (TP * HEAD)) + EPS)
    first = res[...] + dot(wot[...], heads) * scale

    def totals(value, stat, send_sem, recv_sem):
        stat[tp] = jnp.concatenate(
            [jnp.sum(value, axis=0, keepdims=True), jnp.sum(value * value, axis=0, keepdims=True)], axis=0
        )

        def tell(k, carry):
            send(stat.at[tp], stat.at[tp], send_sem.at[k], recv_sem.at[k], {"tp": lax.rem(tp + k, TP)})
            return carry

        def hear(k, carry):
            arrived(stat.at[lax.rem(tp + TP - k, TP)], send_sem.at[k], recv_sem.at[k], {"tp": lax.rem(tp + k, TP)})
            return carry

        lax.fori_loop(1, TP, tell, 0)
        lax.fori_loop(1, TP, hear, 0)
        total = jnp.sum(stat[...], axis=0)
        center = total[0:1] * (1.0 / D)
        spread = total[1:2] * (1.0 / D) - center * center
        return center, lax.rsqrt(spread + EPS)

    center, scale = totals(first, stat1, s_send, s_recv)
    hidden = (first - center) * scale * gain1 + shift1
    hid[...] = hidden

    packed = dot_nt(select[...], hidden.astype(BF))
    going[...] = packed.reshape(SP, CAP, COLS).astype(BF)
    own = pltpu.make_async_copy(going.at[sp], came.at[sp], own_sem.at[0])
    own.start()

    def out_go(k, carry):
        to = lax.rem(sp + k, SP)
        send(going.at[to], came.at[sp], d_send.at[k], d_recv.at[k], {"sp": to})
        return carry

    def out_come(k, carry):
        source = lax.rem(sp + SP - k, SP)
        arrived(came.at[source], d_send.at[k], d_recv.at[k], {"sp": lax.rem(sp + k, SP)})
        return carry

    lax.fori_loop(1, SP, out_go, 0)
    w_copies[0].wait()
    w_copies[1].wait()
    lax.fori_loop(1, SP, out_come, 0)
    own.wait()

    for half in range(2):
        block = came[16 * half : 16 * half + 16].astype(F32).reshape(HALF, COLS)
        grid[tp, half] = block.astype(BF)

    def piece(owner, half, core):
        return grid.at[chip(owner) * 2 + core, half]

    def ring_send(m, lanes):
        hops, half = lanes[m]
        if lanes is RIGHT:
            p = piece(NY - hops, half, c)
            send(p, p, gr_send.at[m], gr_recv.at[m], on_y(1))
        else:
            p = piece(hops, half, c)
            send(p, p, gl_send.at[m], gl_recv.at[m], on_y(NY - 1))

    def share_send(index, p):
        send(p, p, gs_send.at[index], gs_recv.at[index], sibling)

    for m in range(2):
        ring_send(m, RIGHT)
        ring_send(m, LEFT)
    for half in range(2):
        share_send(half, piece(0, half, c))

    def multiply(owner, half, fresh):
        at = chip(owner)
        both = jnp.concatenate([grid[at * 2, half], grid[at * 2 + 1, half]], axis=1)
        product = dot(both, wgu[pl.ds(pl.multiple_of(at * 256, 256), 256), :])
        if fresh:
            acc[half] = product
        else:
            acc[half] += product

    for half in range(2):
        arrived(piece(0, half, 1 - c), gs_send.at[half], gs_recv.at[half], sibling)
        multiply(0, half, True)
    waiting = []
    for m in range(7):
        now = []
        for lanes in (RIGHT, LEFT):
            hops, half = lanes[m]
            right = lanes is RIGHT
            owner = NY - 1 - hops if right else hops + 1
            p = piece(owner, half, c)
            s, r = (gr_send, gr_recv) if right else (gl_send, gl_recv)
            arrived(p, s.at[m], r.at[m], on_y(1 if right else NY - 1))
            if m + 2 < 7:
                ring_send(m + 2, lanes)
            index = 2 + 2 * m + (0 if right else 1)
            share_send(index, p)
            now.append((owner, half, index))
        for owner, half, index in waiting:
            arrived(piece(owner, half, 1 - c), gs_send.at[index], gs_recv.at[index], sibling)
            multiply(owner, half, False)
        waiting = now
    for owner, half, index in waiting:
        arrived(piece(owner, half, 1 - c), gs_send.at[index], gs_recv.at[index], sibling)
        multiply(owner, half, False)
    for copy in w_copies[2:]:
        copy.wait()
    for half in range(2):
        gate, up = acc[half, :, 0:FFB], acc[half, :, FFB:]
        mid[half] = (gate / (1.0 + jnp.exp(-gate)) * up).astype(BF)

    def partials(i):
        for half in range(2):
            product = dot(mid[half], wd[chip(DESTS[i])])
            mine[i, half] = product[:, 0:COLS]
            sib_out[i, half] = product[:, COLS:].astype(BF)
        send(sib_out.at[i], sib_in.at[i], rs_send.at[i], rs_recv.at[i], sibling)

    def paired(i):
        arrived(sib_in.at[i], rs_send.at[i], rs_recv.at[i], sibling)

    def summed(i, half):
        return mine[i, half] + sib_in[i, half].astype(F32)

    def pass_on(m):
        for lanes, o, n, s, r, d in (
            (SUM_RIGHT, right_out, right_in, rr_send, rr_recv, 1),
            (SUM_LEFT, left_out, left_in, rl_send, rl_recv, NY - 1),
        ):
            i, half = lanes[m]
            value = summed(i, half)
            if m >= 2:
                arrived(n.at[m - 2], s.at[m - 2], r.at[m - 2], on_y(d))
                value = value + n[m - 2].astype(F32)
            o[m] = value.astype(BF)
            send(o.at[m], n.at[m], s.at[m], r.at[m], on_y(d))

    partials(0)
    partials(1)
    partials(2)
    paired(0)
    pass_on(0)
    paired(1)
    paired(2)
    pass_on(1)
    partials(3)
    partials(4)
    pass_on(2)
    paired(3)
    paired(4)
    pass_on(3)
    partials(5)
    partials(6)
    pass_on(4)
    paired(5)
    paired(6)
    pass_on(5)
    partials(7)
    pass_on(6)
    paired(7)
    for m in (5, 6):
        arrived(right_in.at[m], rr_send.at[m], rr_recv.at[m], on_y(1))
        arrived(left_in.at[m], rl_send.at[m], rl_recv.at[m], on_y(NY - 1))
    for half in range(2):
        value = summed(7, half) + right_in[6 - half].astype(F32) + left_in[5 + half].astype(F32)
        back_out[16 * half : 16 * half + 16] = value.reshape(16, CAP, COLS).astype(BF)

    own2 = pltpu.make_async_copy(back_out.at[sp], back_in.at[sp], own_sem.at[1])
    own2.start()

    def back_go(k, carry):
        to = lax.rem(sp + k, SP)
        send(back_out.at[to], back_in.at[sp], b_send.at[k], b_recv.at[k], {"sp": to})
        return carry

    def back_come(k, carry):
        source = lax.rem(sp + SP - k, SP)
        arrived(back_in.at[source], b_send.at[k], b_recv.at[k], {"sp": lax.rem(sp + k, SP)})
        return carry

    lax.fori_loop(1, SP, back_go, 0)
    gain2, shift2 = twice(column(final_gain[...])), twice(column(final_shift[...]))
    lax.fori_loop(1, SP, back_come, 0)
    own2.wait()

    returned = jnp.transpose(back_in[...].astype(F32).reshape(ROWS, COLS)).astype(BF)
    moe = dot(returned, mix_hi[...]) + dot(returned, mix_lo[...])
    second = ALPHA * hid[...] + moe
    center, scale = totals(second, stat2, s2_send, s2_recv)
    out[...] = jnp.transpose((second - center) * scale * gain2 + shift2).astype(BF)

    for i in range(3):
        left_here((tail_k, tail_v, tail_d)[i], tail_sem.at[i], tail_sem.at[3 + i], after)
    for k in range(1, NY):
        left_here(att.at[tp], a_send.at[k], a_recv.at[k], on_y(k))
    for k in range(NY):
        left_here(att.at[tp], as_send.at[k], as_recv.at[k], sibling)

    def stats_left(k, carry):
        left_here(stat1.at[tp], s_send.at[k], s_recv.at[k], {"tp": lax.rem(tp + k, TP)})
        left_here(stat2.at[tp], s2_send.at[k], s2_recv.at[k], {"tp": lax.rem(tp + k, TP)})
        return carry

    def rows_left(k, carry):
        to = lax.rem(sp + k, SP)
        left_here(going.at[to], d_send.at[k], d_recv.at[k], {"sp": to})
        left_here(back_out.at[to], b_send.at[k], b_recv.at[k], {"sp": to})
        return carry

    lax.fori_loop(1, TP, stats_left, 0)
    lax.fori_loop(1, SP, rows_left, 0)
    for m in range(7):
        left_here(grid.at[0, 0], gr_send.at[m], gr_recv.at[m], on_y(1))
        left_here(grid.at[0, 0], gl_send.at[m], gl_recv.at[m], on_y(NY - 1))
        left_here(right_out.at[m], rr_send.at[m], rr_recv.at[m], on_y(1))
        left_here(left_out.at[m], rl_send.at[m], rl_recv.at[m], on_y(NY - 1))
    for index in range(16):
        left_here(grid.at[0, 0], gs_send.at[index], gs_recv.at[index], sibling)
    for i in range(NY):
        left_here(sib_out.at[i], rs_send.at[i], rs_recv.at[i], sibling)


def local(
    residual, queries, keys, values, documents, sinks, head_gain, out_weight, norm_gain, norm_shift,
    routes, route_logits, gate_weight, up_weight, down_weight, final_gain, final_shift,
):
    vmem = pl.BlockSpec(memory_space=pltpu.VMEM)
    smem = pl.BlockSpec(memory_space=pltpu.SMEM)
    hbm = pl.BlockSpec(memory_space=pl.ANY)
    dma = pltpu.SemaphoreType.DMA
    return pl.pallas_call(
        kernel,
        out_shape=jax.ShapeDtypeStruct((TOK, COLS), BF),
        in_specs=[vmem] * 5 + [smem] + [vmem] * 8 + [hbm] * 3,
        out_specs=vmem,
        scratch_shapes=[
            pltpu.VMEM((D, 2 * FFB), BF),
            pltpu.VMEM((NY, FFB, 2 * COLS), BF),
            pltpu.VMEM((WINDOW, 128), BF),
            pltpu.VMEM((WINDOW, 128), BF),
            pltpu.VMEM((1, WINDOW), jnp.int32),
            pltpu.VMEM((COLS, TP * HEAD), BF),
            pltpu.VMEM((COLS, TOK), F32),
            pltpu.VMEM((128, WINDOW + TOK), BF),
            pltpu.VMEM((ROWS, TOK), BF),
            pltpu.VMEM((ROWS, TOK), BF),
            pltpu.VMEM((ROWS, TOK), BF),
            pltpu.VMEM((TP, HEAD, TOK), BF),
            pltpu.VMEM((TP, 2, TOK), F32),
            pltpu.VMEM((TP, 2, TOK), F32),
            pltpu.VMEM((COLS, TOK), F32),
            pltpu.VMEM((SP, CAP, COLS), BF),
            pltpu.VMEM((SP, CAP, COLS), BF),
            pltpu.VMEM((TP, 2, HALF, COLS), BF),
            pltpu.VMEM((2, HALF, 2 * FFB), F32),
            pltpu.VMEM((2, HALF, FFB), BF),
            pltpu.VMEM((NY, 2, HALF, COLS), F32),
            pltpu.VMEM((NY, 2, HALF, COLS), BF),
            pltpu.VMEM((NY, 2, HALF, COLS), BF),
            pltpu.VMEM((7, HALF, COLS), BF),
            pltpu.VMEM((7, HALF, COLS), BF),
            pltpu.VMEM((7, HALF, COLS), BF),
            pltpu.VMEM((7, HALF, COLS), BF),
            pltpu.VMEM((SP, CAP, COLS), BF),
            pltpu.VMEM((SP, CAP, COLS), BF),
            dma((2 + 2 * NY,)),
            dma((6,)),
            dma((NY,)), dma((NY,)), dma((NY,)), dma((NY,)),
            dma((TP,)), dma((TP,)), dma((TP,)), dma((TP,)),
            dma((SP,)), dma((SP,)),
            dma((7,)), dma((7,)), dma((7,)), dma((7,)), dma((16,)), dma((16,)),
            dma((NY,)), dma((NY,)), dma((7,)), dma((7,)), dma((7,)), dma((7,)),
            dma((SP,)), dma((SP,)), dma((2,)),
        ],
        compiler_params=pltpu.CompilerParams(
            collective_id=0, has_side_effects=True, vmem_limit_bytes=60 * 1024 * 1024
        ),
        name="layer",
    )(
        residual, queries.T, keys, values, documents.reshape(1, TOK), sinks.reshape(1, 1),
        head_gain.reshape(1, TP * HEAD), out_weight, norm_gain.reshape(1, COLS), norm_shift.reshape(1, COLS),
        routes.T, route_logits.T, final_gain.reshape(1, COLS), final_shift.reshape(1, COLS),
        gate_weight, up_weight, down_weight,
    )


def solution(mesh):
    return jax.shard_map(
        local,
        mesh=mesh,
        in_specs=(
            P("sp", "tp"), P("sp", "tp"), P("sp", None), P("sp", None), P("sp"), P("tp"), P(), P(None, "tp"),
            P("tp"), P("tp"), P("sp", None), P("sp", None), P("sp", None, "tp"), P("sp", None, "tp"),
            P("sp", "tp", None), P("tp"), P("tp"),
        ),
        out_specs=P("sp", "tp"),
        check_vma=False,
    )
```

```python
import jax
import jax.numpy as jnp
from jax import lax
from jax.experimental import pallas as pl
from jax.experimental.pallas import tpu as pltpu
from jax.sharding import PartitionSpec as P

D = 2048
HEAD = 64
WINDOW = 128
TOK = 256
CAP = 24
SP = 32
TP = 16
NY = 8
COLS = D // TP
ROWS = SP * CAP
HALF = ROWS // 2
FFB = 384
ALPHA = 8.0**0.25
EPS = 1e-05
MESH = pl.DeviceIdType.MESH
BF = jnp.bfloat16
F32 = jnp.float32

RIGHT = [(0, 0), (0, 1), (1, 0), (1, 1), (2, 0), (2, 1), (3, 0)]
LEFT = [(0, 1), (0, 0), (1, 1), (1, 0), (2, 1), (2, 0), (3, 1)]
DESTS = [4, 3, 5, 2, 6, 1, 7, 0]
SUM_RIGHT = [(0, 0), (1, 1), (1, 0), (3, 1), (3, 0), (5, 1), (5, 0)]
SUM_LEFT = [(0, 1), (2, 0), (2, 1), (4, 0), (4, 1), (6, 0), (6, 1)]


def dot(a, b):
    return lax.dot_general(a, b, (((1,), (0,)), ((), ())), preferred_element_type=F32)


def dot_nt(a, b):
    return lax.dot_general(a, b, (((1,), (1,)), ((), ())), preferred_element_type=F32)


def column(row):
    return jnp.transpose(jnp.broadcast_to(row, (128, 128)))


def twice(a):
    return jnp.concatenate([a, a], axis=1)


def kernel(
    residual_hbm, queries_hbm, keys_hbm, values_hbm, docs_hbm, sinks_hbm, head_gain_hbm, out_weight_hbm,
    norm_gain_hbm, norm_shift_hbm, routes_hbm, logits_hbm, final_gain_hbm, final_shift_hbm,
    gate_hbm, up_hbm, down_hbm,
    out,
    residual, queries, keys, values, docs, sinks, head_gain, out_weight, norm_gain, norm_shift,
    routes, logits, final_gain, final_shift,
    wgu, wd, tail_k, tail_v, tail_d, wot, res, vt, select, mix_hi, mix_lo,
    att, stat1, stat2, hid, going, came, grid, acc, mid, mine, sib_out, sib_in,
    right_out, right_in, left_out, left_in, back_out, back_in,
    in_sem, w_sem, tail_sem, a_send, a_recv, as_send, as_recv, s_send, s_recv,
    d_send, d_recv, gr_send, gr_recv, gl_send, gl_recv, gs_send, gs_recv,
    rs_send, rs_recv, rr_send, rr_recv, rl_send, rl_recv, b_send, b_recv, own_sem,
):
    sp = lax.axis_index("sp")
    tp = lax.axis_index("tp")
    y = lax.div(tp, 2)
    c = lax.rem(tp, 2)
    sibling = {"tp": y * 2 + 1 - c}

    def chip(distance):
        return lax.rem(y + distance, NY)

    def on_y(distance):
        return {"tp": chip(distance) * 2 + c}

    def send(src, dst, send_sem, recv_sem, device):
        pltpu.make_async_remote_copy(
            src_ref=src, dst_ref=dst, send_sem=send_sem, recv_sem=recv_sem,
            device_id=device, device_id_type=MESH,
        ).start()

    def arrived(dst, send_sem, recv_sem, device):
        pltpu.make_async_remote_copy(
            src_ref=dst, dst_ref=dst, send_sem=send_sem, recv_sem=recv_sem,
            device_id=device, device_id_type=MESH,
        ).wait_recv()

    def left_here(src, send_sem, recv_sem, device):
        pltpu.make_async_remote_copy(
            src_ref=src, dst_ref=src, send_sem=send_sem, recv_sem=recv_sem,
            device_id=device, device_id_type=MESH,
        ).wait_send()

    barrier = pltpu.get_barrier_semaphore()

    def greet_tp(k, carry):
        pl.semaphore_signal(barrier, inc=1, device_id={"tp": lax.rem(tp + k, TP)}, device_id_type=MESH)
        return carry

    def greet_sp(k, carry):
        pl.semaphore_signal(barrier, inc=1, device_id={"sp": lax.rem(sp + k, SP)}, device_id_type=MESH)
        return carry

    lax.fori_loop(1, TP, greet_tp, 0)
    lax.fori_loop(1, SP, greet_sp, 0)
    inputs = [
        (queries_hbm, queries), (keys_hbm, keys), (docs_hbm, docs), (sinks_hbm, sinks), (values_hbm, values),
        (out_weight_hbm, out_weight), (head_gain_hbm, head_gain), (residual_hbm, residual),
        (routes_hbm, routes), (logits_hbm, logits), (norm_gain_hbm, norm_gain), (norm_shift_hbm, norm_shift),
        (final_gain_hbm, final_gain), (final_shift_hbm, final_shift),
    ]
    in_copies = [pltpu.make_async_copy(src, dst, in_sem.at[i]) for i, (src, dst) in enumerate(inputs)]
    for copy in in_copies:
        copy.start()
    w_copies = [
        pltpu.make_async_copy(gate_hbm.at[0], wgu.at[:, 0:FFB], w_sem.at[0]),
        pltpu.make_async_copy(up_hbm.at[0], wgu.at[:, FFB : 2 * FFB], w_sem.at[1]),
    ]
    for d in range(NY):
        for part in range(2):
            block = 2 * d + (c if part == 0 else 1 - c)
            w_copies.append(
                pltpu.make_async_copy(
                    down_hbm.at[0, :, pl.ds(pl.multiple_of(block * 128, 128), 128)],
                    wd.at[d, :, 128 * part : 128 * part + 128],
                    w_sem.at[2],
                )
            )
    for copy in w_copies:
        copy.start()
    for copy in in_copies[:5]:
        copy.wait()

    upper = tp >= TP // 2
    vt[:, WINDOW:] = jnp.transpose(values[...].astype(F32)).astype(BF)
    qt = queries[...]
    zero_q = jnp.zeros_like(qt)
    q_wide = jnp.concatenate([jnp.where(upper, zero_q, qt), jnp.where(upper, qt, zero_q)], axis=0)
    doc_row = docs[...].astype(F32)
    sink = sinks[...]

    def attend(key_rows, v_cols, key_docs, begin):
        score = dot(key_rows, q_wide[:, begin : begin + 128]) * HEAD ** (-0.5)
        ahead = (
            WINDOW
            + lax.broadcasted_iota(jnp.int32, (256, 128), 1)
            - lax.broadcasted_iota(jnp.int32, (256, 128), 0)
        )
        allowed = (ahead >= 0) & (ahead < WINDOW) & (key_docs == doc_row[:, begin : begin + 128])
        score = jnp.where(allowed, score, -1e30)
        top = jnp.maximum(jnp.max(score, axis=0, keepdims=True), sink)
        e = jnp.exp(score - top)
        total = jnp.sum(e, axis=0, keepdims=True) + jnp.exp(sink - top)
        probs = (e * (1.0 / total)).astype(BF)
        wide = dot(v_cols, probs)
        return jnp.where(upper, wide[HEAD:, :], wide[:HEAD, :]).astype(BF)

    docs0 = column(doc_row[:, 0:128])
    docs1 = column(doc_row[:, 128:256])
    att[1, y, c] = attend(keys[...], vt[:, 128:384], jnp.concatenate([docs0, docs1], axis=0), 128)

    pl.semaphore_wait(barrier, TP - 1 + SP - 1)

    after = {"sp": lax.rem(sp + 1, SP)}
    send(keys.at[128:256], tail_k, tail_sem.at[0], tail_sem.at[3], after)
    send(values.at[128:256], tail_v, tail_sem.at[1], tail_sem.at[4], after)
    send(docs.at[:, 128:256], tail_d, tail_sem.at[2], tail_sem.at[5], after)

    def heads_go(block):
        for k in (4, 3, 5, 2, 6, 1, 7):
            send(att.at[block, y, c], att.at[block, y, c], a_send.at[block], a_recv.at[block], on_y(k))

    heads_go(1)

    for copy in in_copies[5:]:
        copy.wait()
    wot[...] = (jnp.transpose(out_weight[...].astype(F32)) * head_gain[...]).astype(BF)
    res[...] = ALPHA * jnp.transpose(residual[...].astype(F32))

    arrived(tail_k, tail_sem.at[0], tail_sem.at[3], after)
    arrived(tail_v, tail_sem.at[1], tail_sem.at[4], after)
    arrived(tail_d, tail_sem.at[2], tail_sem.at[5], after)
    vt[:, 0:WINDOW] = jnp.transpose(tail_v[...].astype(F32)).astype(BF)
    before_docs = jnp.where(sp > 0, tail_d[...].astype(F32), -1.0)
    att[0, y, c] = attend(
        jnp.concatenate([tail_k[...], keys[0:128, :]], axis=0),
        vt[:, 0:256],
        jnp.concatenate([column(before_docs), docs0], axis=0),
        0,
    )

    heads_go(0)

    r0, r1 = routes[0:1, :], routes[1:2, :]
    experts = lax.broadcasted_iota(jnp.int32, (SP, TOK), 0)
    first_hit, second_hit = r0 == experts, r1 == experts
    named = jnp.where(first_hit | second_hit, 1.0, 0.0)
    earlier = jnp.where(
        lax.broadcasted_iota(jnp.int32, (TOK, TOK), 0) < lax.broadcasted_iota(jnp.int32, (TOK, TOK), 1), 1.0, 0.0
    ).astype(BF)
    place = jnp.where(named > 0.0, dot(named.astype(BF), earlier), -1.0)
    l0, l1 = logits[0:1, :], logits[1:2, :]
    l_top = jnp.maximum(l0, l1)
    e0, e1 = jnp.exp(l0 - l_top), jnp.exp(l1 - l_top)
    per = 1.0 / (e0 + e1)
    share = jnp.where(first_hit, e0 * per, jnp.where(second_hit, e1 * per, 0.0))
    slots = lax.broadcasted_iota(jnp.int32, (CAP, TOK), 0).astype(F32)
    for group in range(4):
        hits, weights = [], []
        for e in range(8 * group, 8 * group + 8):
            hit = place[e : e + 1, :] == slots
            hits.append(jnp.where(hit, 1.0, 0.0))
            weights.append(jnp.where(hit, share[e : e + 1, :], 0.0))
        rows = pl.ds(group * 8 * CAP, 8 * CAP)
        weight = jnp.concatenate(weights, axis=0)
        high = weight.astype(BF)
        select[rows, :] = jnp.concatenate(hits, axis=0).astype(BF)
        mix_hi[rows, :] = high
        mix_lo[rows, :] = (weight - high.astype(F32)).astype(BF)
    gain1, shift1 = twice(column(norm_gain[...])), twice(column(norm_shift[...]))

    for block in (1, 0):
        arrived(att.at[block, 0:7, c], a_send.at[block], a_recv.at[block], on_y(1))
        send(att.at[block, :, c], att.at[block, :, c], as_send.at[block], as_recv.at[block], sibling)
    first = []
    for block in (1, 0):
        arrived(att.at[block, :, 1 - c], as_send.at[block], as_recv.at[block], sibling)
        heads = att[block].reshape(TP * HEAD, 128)
        wide = heads.astype(F32)
        scale = lax.rsqrt(jnp.sum(wide * wide, axis=0, keepdims=True) * (1.0 / (TP * HEAD)) + EPS)
        first.append(res[:, 128 * block : 128 * block + 128] + dot(wot[...], heads) * scale)
    first = jnp.concatenate([first[1], first[0]], axis=1)

    def totals(value, stat, send_sem, recv_sem):
        stat[tp] = jnp.concatenate(
            [jnp.sum(value, axis=0, keepdims=True), jnp.sum(value * value, axis=0, keepdims=True)], axis=0
        )

        def tell(k, carry):
            send(stat.at[tp], stat.at[tp], send_sem, recv_sem, {"tp": lax.rem(tp + k, TP)})
            return carry

        lax.fori_loop(1, TP, tell, 0)
        arrived(stat.at[0 : TP - 1], send_sem, recv_sem, sibling)
        total = jnp.sum(stat[...], axis=0)
        center = total[0:1] * (1.0 / D)
        spread = total[1:2] * (1.0 / D) - center * center
        return center, lax.rsqrt(spread + EPS)

    center, scale = totals(first, stat1, s_send.at[0], s_recv.at[0])
    hidden = (first - center) * scale * gain1 + shift1
    hid[...] = hidden

    packed = dot_nt(select[...], hidden.astype(BF))
    going[...] = packed.reshape(SP, CAP, COLS).astype(BF)
    own = pltpu.make_async_copy(going.at[sp], came.at[sp], own_sem.at[0])
    own.start()

    def out_go(k, carry):
        to = lax.rem(sp + k, SP)
        send(going.at[to], came.at[sp], d_send.at[0], d_recv.at[0], {"sp": to})
        return carry

    lax.fori_loop(1, SP, out_go, 0)
    w_copies[0].wait()
    w_copies[1].wait()
    arrived(came.at[0 : SP - 1], d_send.at[0], d_recv.at[0], after)
    own.wait()

    for half in range(2):
        block = came[16 * half : 16 * half + 16].astype(F32).reshape(HALF, COLS)
        grid[tp, half] = block.astype(BF)

    def piece(owner, half, core):
        return grid.at[chip(owner) * 2 + core, half]

    def ring_send(m, lanes):
        hops, half = lanes[m]
        if lanes is RIGHT:
            p = piece(NY - hops, half, c)
            send(p, p, gr_send.at[0], gr_recv.at[m], on_y(1))
        else:
            p = piece(hops, half, c)
            send(p, p, gl_send.at[0], gl_recv.at[m], on_y(NY - 1))

    def share_send(index, p):
        send(p, p, gs_send.at[0], gs_recv.at[index], sibling)

    for m in range(2):
        ring_send(m, RIGHT)
        ring_send(m, LEFT)
    for half in range(2):
        share_send(half, piece(0, half, c))

    def multiply(owner, half, fresh):
        at = chip(owner)
        both = jnp.concatenate([grid[at * 2, half], grid[at * 2 + 1, half]], axis=1)
        product = dot(both, wgu[pl.ds(pl.multiple_of(at * 256, 256), 256), :])
        if fresh:
            acc[half] = product
        else:
            acc[half] += product

    for half in range(2):
        arrived(piece(0, half, 1 - c), gs_send.at[0], gs_recv.at[half], sibling)
        multiply(0, half, True)
    waiting = []
    for m in range(7):
        now = []
        for lanes in (RIGHT, LEFT):
            hops, half = lanes[m]
            right = lanes is RIGHT
            owner = NY - 1 - hops if right else hops + 1
            p = piece(owner, half, c)
            s, r = (gr_send, gr_recv) if right else (gl_send, gl_recv)
            arrived(p, s.at[0], r.at[m], on_y(1 if right else NY - 1))
            if m + 2 < 7:
                ring_send(m + 2, lanes)
            index = 2 + 2 * m + (0 if right else 1)
            share_send(index, p)
            now.append((owner, half, index))
        for owner, half, index in waiting:
            arrived(piece(owner, half, 1 - c), gs_send.at[0], gs_recv.at[index], sibling)
            multiply(owner, half, False)
        waiting = now
    for owner, half, index in waiting:
        arrived(piece(owner, half, 1 - c), gs_send.at[0], gs_recv.at[index], sibling)
        multiply(owner, half, False)
    pltpu.make_async_copy(wd, wd, w_sem.at[2]).wait()
    for half in range(2):
        gate, up = acc[half, :, 0:FFB], acc[half, :, FFB:]
        mid[half] = (gate / (1.0 + jnp.exp(-gate)) * up).astype(BF)

    def partials(i):
        for half in range(2):
            product = dot(mid[half], wd[chip(DESTS[i])])
            mine[i, half] = product[:, 0:COLS]
            sib_out[i, half] = product[:, COLS:].astype(BF)
        send(sib_out.at[i], sib_in.at[i], rs_send.at[0], rs_recv.at[i], sibling)

    def paired(i):
        arrived(sib_in.at[i], rs_send.at[0], rs_recv.at[i], sibling)

    def summed(i, half):
        return mine[i, half] + sib_in[i, half].astype(F32)

    def pass_on(m):
        for lanes, o, n, s, r, d in (
            (SUM_RIGHT, right_out, right_in, rr_send, rr_recv, 1),
            (SUM_LEFT, left_out, left_in, rl_send, rl_recv, NY - 1),
        ):
            i, half = lanes[m]
            value = summed(i, half)
            if m >= 2:
                arrived(n.at[m - 2], s.at[0], r.at[m - 2], on_y(d))
                value = value + n[m - 2].astype(F32)
            o[m] = value.astype(BF)
            send(o.at[m], n.at[m], s.at[0], r.at[m], on_y(d))

    partials(0)
    partials(1)
    partials(2)
    paired(0)
    pass_on(0)
    paired(1)
    paired(2)
    pass_on(1)
    partials(3)
    partials(4)
    pass_on(2)
    paired(3)
    paired(4)
    pass_on(3)
    partials(5)
    partials(6)
    pass_on(4)
    paired(5)
    paired(6)
    pass_on(5)
    partials(7)
    pass_on(6)
    paired(7)
    for m in (5, 6):
        arrived(right_in.at[m], rr_send.at[0], rr_recv.at[m], on_y(1))
        arrived(left_in.at[m], rl_send.at[0], rl_recv.at[m], on_y(NY - 1))
    for half in range(2):
        value = summed(7, half) + right_in[6 - half].astype(F32) + left_in[5 + half].astype(F32)
        back_out[16 * half : 16 * half + 16] = value.reshape(16, CAP, COLS).astype(BF)

    own2 = pltpu.make_async_copy(back_out.at[sp], back_in.at[sp], own_sem.at[1])
    own2.start()

    def back_go(k, carry):
        to = lax.rem(sp + k, SP)
        send(back_out.at[to], back_in.at[sp], b_send.at[0], b_recv.at[0], {"sp": to})
        return carry

    lax.fori_loop(1, SP, back_go, 0)
    gain2, shift2 = twice(column(final_gain[...])), twice(column(final_shift[...]))
    arrived(back_in.at[0 : SP - 1], b_send.at[0], b_recv.at[0], after)
    own2.wait()

    returned = jnp.transpose(back_in[...].astype(F32).reshape(ROWS, COLS)).astype(BF)
    moe = dot(returned, mix_hi[...]) + dot(returned, mix_lo[...])
    second = ALPHA * hid[...] + moe
    center, scale = totals(second, stat2, s_send.at[1], s_recv.at[1])
    out[...] = jnp.transpose((second - center) * scale * gain2 + shift2).astype(BF)

    for i in range(3):
        left_here((tail_k, tail_v, tail_d)[i], tail_sem.at[i], tail_sem.at[3 + i], after)
    for block in range(2):
        left_here(att.at[block, 0:7, 0], a_send.at[block], a_recv.at[block], on_y(1))
        left_here(att.at[block, :, 0], as_send.at[block], as_recv.at[block], sibling)
        left_here(stat1.at[0 : TP - 1], s_send.at[block], s_recv.at[block], sibling)
    left_here(going.at[0 : SP - 1], d_send.at[0], d_recv.at[0], after)
    left_here(back_out.at[0 : SP - 1], b_send.at[0], b_recv.at[0], after)
    left_here(right_out, gr_send.at[0], gr_recv.at[0], on_y(1))
    left_here(left_out, gl_send.at[0], gl_recv.at[0], on_y(NY - 1))
    left_here(right_out, rr_send.at[0], rr_recv.at[0], on_y(1))
    left_here(left_out, rl_send.at[0], rl_recv.at[0], on_y(NY - 1))
    left_here(sib_out, gs_send.at[0], gs_recv.at[0], sibling)
    left_here(sib_out, rs_send.at[0], rs_recv.at[0], sibling)


def local(
    residual, queries, keys, values, documents, sinks, head_gain, out_weight, norm_gain, norm_shift,
    routes, route_logits, gate_weight, up_weight, down_weight, final_gain, final_shift,
):
    vmem = pl.BlockSpec(memory_space=pltpu.VMEM)
    hbm = pl.BlockSpec(memory_space=pl.ANY)
    dma = pltpu.SemaphoreType.DMA
    return pl.pallas_call(
        kernel,
        out_shape=pltpu.VMEM((TOK, COLS), BF),
        in_specs=[hbm] * 17,
        out_specs=vmem,
        scratch_shapes=[
            pltpu.VMEM((TOK, COLS), BF),
            pltpu.VMEM((HEAD, TOK), BF),
            pltpu.VMEM((TOK, 128), BF),
            pltpu.VMEM((TOK, 128), BF),
            pltpu.VMEM((1, TOK), jnp.int32),
            pltpu.VMEM((1, 1), F32),
            pltpu.VMEM((1, TP * HEAD), F32),
            pltpu.VMEM((TP * HEAD, COLS), BF),
            pltpu.VMEM((1, COLS), F32),
            pltpu.VMEM((1, COLS), F32),
            pltpu.VMEM((2, TOK), jnp.int32),
            pltpu.VMEM((2, TOK), F32),
            pltpu.VMEM((1, COLS), F32),
            pltpu.VMEM((1, COLS), F32),
            pltpu.VMEM((D, 2 * FFB), BF),
            pltpu.VMEM((NY, FFB, 2 * COLS), BF),
            pltpu.VMEM((WINDOW, 128), BF),
            pltpu.VMEM((WINDOW, 128), BF),
            pltpu.VMEM((1, WINDOW), jnp.int32),
            pltpu.VMEM((COLS, TP * HEAD), BF),
            pltpu.VMEM((COLS, TOK), F32),
            pltpu.VMEM((128, WINDOW + TOK), BF),
            pltpu.VMEM((ROWS, TOK), BF),
            pltpu.VMEM((ROWS, TOK), BF),
            pltpu.VMEM((ROWS, TOK), BF),
            pltpu.VMEM((2, NY, 2, HEAD, 128), BF),
            pltpu.VMEM((TP, 2, TOK), F32),
            pltpu.VMEM((TP, 2, TOK), F32),
            pltpu.VMEM((COLS, TOK), F32),
            pltpu.VMEM((SP, CAP, COLS), BF),
            pltpu.VMEM((SP, CAP, COLS), BF),
            pltpu.VMEM((TP, 2, HALF, COLS), BF),
            pltpu.VMEM((2, HALF, 2 * FFB), F32),
            pltpu.VMEM((2, HALF, FFB), BF),
            pltpu.VMEM((NY, 2, HALF, COLS), F32),
            pltpu.VMEM((NY, 2, HALF, COLS), BF),
            pltpu.VMEM((NY, 2, HALF, COLS), BF),
            pltpu.VMEM((7, HALF, COLS), BF),
            pltpu.VMEM((7, HALF, COLS), BF),
            pltpu.VMEM((7, HALF, COLS), BF),
            pltpu.VMEM((7, HALF, COLS), BF),
            pltpu.VMEM((SP, CAP, COLS), BF),
            pltpu.VMEM((SP, CAP, COLS), BF),
            dma((14,)), dma((3,)), dma((6,)),
            dma((2,)), dma((2,)), dma((2,)), dma((2,)), dma((2,)), dma((2,)),
            dma((1,)), dma((1,)),
            dma((1,)), dma((7,)), dma((1,)), dma((7,)), dma((1,)), dma((16,)),
            dma((1,)), dma((NY,)), dma((1,)), dma((7,)), dma((1,)), dma((7,)),
            dma((1,)), dma((1,)), dma((2,)),
        ],
        compiler_params=pltpu.CompilerParams(
            collective_id=0, has_side_effects=True, vmem_limit_bytes=60 * 1024 * 1024
        ),
        name="layer",
    )(
        residual, queries.T, keys, values, documents.reshape(1, TOK), sinks.reshape(1, 1),
        head_gain.reshape(1, TP * HEAD), out_weight, norm_gain.reshape(1, COLS), norm_shift.reshape(1, COLS),
        routes.T, route_logits.T, final_gain.reshape(1, COLS), final_shift.reshape(1, COLS),
        gate_weight, up_weight, down_weight,
    )


def solution(mesh):
    return jax.shard_map(
        local,
        mesh=mesh,
        in_specs=(
            P("sp", "tp"), P("sp", "tp"), P("sp", None), P("sp", None), P("sp"), P("tp"), P(), P(None, "tp"),
            P("tp"), P("tp"), P("sp", None), P("sp", None), P("sp", None, "tp"), P("sp", None, "tp"),
            P("sp", "tp", None), P("tp"), P("tp"),
        ),
        out_specs=P("sp", "tp"),
        check_vma=False,
    )
```

```python
import jax
import jax.numpy as jnp
from jax import lax
from jax.experimental import pallas as pl
from jax.experimental.pallas import tpu as pltpu
from jax.sharding import PartitionSpec as P

D = 2048
HEAD = 64
WINDOW = 128
TOK = 256
CAP = 24
SP = 32
TP = 16
NY = 8
COLS = D // TP
ROWS = SP * CAP
HALF = ROWS // 2
FFB = 384
ALPHA = 8.0**0.25
EPS = 1e-05
MESH = pl.DeviceIdType.MESH
BF = jnp.bfloat16
F32 = jnp.float32

QUARTER = ROWS // 4
PLACES = sorted(
    [(dz, dx) for dz in range(8) for dx in range(4)], key=lambda p: min(p[0], 8 - p[0]) + min(p[1], 4 - p[1])
)


def gather_order(near, near_too, far, far_too):
    return [
        (0, near), (0, near_too), (1, near), (1, near_too), (0, far), (0, far_too), (2, near), (2, near_too),
        (1, far), (1, far_too), (3, near), (2, far), (2, far_too), (3, far),
    ]


def sum_order(near, near_too, far, far_too):
    return [
        (4, near), (3, near_too), (3, near), (4, far), (3, far_too), (2, near_too), (3, far), (2, near),
        (2, far_too), (2, far), (1, near_too), (1, far_too), (1, far), (1, near),
    ]


RIGHT, LEFT = gather_order(0, 1, 2, 3), gather_order(1, 0, 3, 2)
SUM_RIGHT, SUM_LEFT = sum_order(0, 1, 2, 3), sum_order(1, 0, 3, 2)
MESSAGES = len(RIGHT)
DESTS = [4, 3, 5, 2, 6, 1, 7, 0]


def dot(a, b):
    return lax.dot_general(a, b, (((1,), (0,)), ((), ())), preferred_element_type=F32)


def dot_nt(a, b):
    return lax.dot_general(a, b, (((1,), (1,)), ((), ())), preferred_element_type=F32)


def column(row):
    return jnp.transpose(jnp.broadcast_to(row, (128, 128)))


def twice(a):
    return jnp.concatenate([a, a], axis=1)


def kernel(
    residual_hbm, queries_hbm, keys_hbm, values_hbm, docs_hbm, sinks_hbm, head_gain_hbm, out_weight_hbm,
    norm_gain_hbm, norm_shift_hbm, routes_hbm, logits_hbm, final_gain_hbm, final_shift_hbm,
    gate_hbm, up_hbm, down_hbm,
    out,
    residual, queries, keys, values, docs, sinks, head_gain, out_weight, norm_gain, norm_shift,
    routes, logits, final_gain, final_shift,
    wgu, wd, tail_k, tail_v, tail_d, wot, res, vt, select, mix_hi, mix_lo, facts, rows_gu,
    att, stat1, stat2, hid, going, came, grid, acc, acc1, acc2, mid, mine, sib_out, sib_in,
    right_out, right_in, left_out, left_in, back_out, back_in,
    in_sem, w_sem, tail_sem, f_send, f_recv, a_send, a_recv, as_send, as_recv, s_send, s_recv,
    d_send, d_recv, gr_send, gr_recv, gl_send, gl_recv, gs_send, gs_recv,
    rs_send, rs_recv, rr_send, rr_recv, rl_send, rl_recv, b_send, b_recv, own_sem,
):
    sp = lax.axis_index("sp")
    tp = lax.axis_index("tp")
    y = lax.div(tp, 2)
    c = lax.rem(tp, 2)
    z = lax.div(sp, 4)
    x = lax.rem(sp, 4)
    sibling = {"tp": y * 2 + 1 - c}

    def chip(distance):
        return lax.rem(y + distance, NY)

    def on_y(distance):
        return {"tp": chip(distance) * 2 + c}

    def send(src, dst, send_sem, recv_sem, device):
        pltpu.make_async_remote_copy(
            src_ref=src, dst_ref=dst, send_sem=send_sem, recv_sem=recv_sem,
            device_id=device, device_id_type=MESH,
        ).start()

    def arrived(dst, send_sem, recv_sem, device):
        pltpu.make_async_remote_copy(
            src_ref=dst, dst_ref=dst, send_sem=send_sem, recv_sem=recv_sem,
            device_id=device, device_id_type=MESH,
        ).wait_recv()

    def left_here(src, send_sem, recv_sem, device):
        pltpu.make_async_remote_copy(
            src_ref=src, dst_ref=src, send_sem=send_sem, recv_sem=recv_sem,
            device_id=device, device_id_type=MESH,
        ).wait_send()

    barrier = pltpu.get_barrier_semaphore()

    inputs = [
        (queries_hbm, queries), (keys_hbm, keys), (docs_hbm, docs), (sinks_hbm, sinks), (values_hbm, values),
        (out_weight_hbm, out_weight), (head_gain_hbm, head_gain), (residual_hbm, residual),
        (routes_hbm, routes), (logits_hbm, logits), (norm_gain_hbm, norm_gain), (norm_shift_hbm, norm_shift),
        (final_gain_hbm, final_gain), (final_shift_hbm, final_shift),
    ]
    in_copies = [pltpu.make_async_copy(src, dst, in_sem.at[i]) for i, (src, dst) in enumerate(inputs)]
    for copy in in_copies[:5]:
        copy.start()

    def greet_tp(k, carry):
        pl.semaphore_signal(barrier, inc=1, device_id={"tp": lax.rem(tp + k, TP)}, device_id_type=MESH)
        return carry

    def greet_sp(k, carry):
        pl.semaphore_signal(barrier, inc=1, device_id={"sp": lax.rem(sp + k, SP)}, device_id_type=MESH)
        return carry

    lax.fori_loop(1, TP, greet_tp, 0)
    lax.fori_loop(1, SP, greet_sp, 0)
    for copy in in_copies[5:]:
        copy.start()
    w_copies = [
        pltpu.make_async_copy(gate_hbm.at[0], wgu.at[:, 0:FFB], w_sem.at[0]),
        pltpu.make_async_copy(up_hbm.at[0], wgu.at[:, FFB : 2 * FFB], w_sem.at[1]),
    ]
    for d in range(NY):
        for part in range(2):
            block = 2 * d + (c if part == 0 else 1 - c)
            w_copies.append(
                pltpu.make_async_copy(
                    down_hbm.at[0, :, pl.ds(pl.multiple_of(block * 128, 128), 128)],
                    wd.at[d, :, 128 * part : 128 * part + 128],
                    w_sem.at[2],
                )
            )
    for copy in in_copies[:5]:
        copy.wait()
    for copy in w_copies:
        copy.start()

    upper = tp >= TP // 2
    vt[:, WINDOW:] = jnp.transpose(values[...].astype(F32)).astype(BF)
    qt = queries[...]
    zero_q = jnp.zeros_like(qt)
    q_wide = jnp.concatenate([jnp.where(upper, zero_q, qt), jnp.where(upper, qt, zero_q)], axis=0)
    doc_row = docs[...].astype(F32)
    sink = sinks[...]

    def attend(key_rows, v_cols, key_docs, begin):
        score = dot(key_rows, q_wide[:, begin : begin + 128]) * HEAD ** (-0.5)
        ahead = (
            WINDOW
            + lax.broadcasted_iota(jnp.int32, (256, 128), 1)
            - lax.broadcasted_iota(jnp.int32, (256, 128), 0)
        )
        allowed = (ahead >= 0) & (ahead < WINDOW) & (key_docs == doc_row[:, begin : begin + 128])
        score = jnp.where(allowed, score, -1e30)
        top = jnp.maximum(jnp.max(score, axis=0, keepdims=True), sink)
        e = jnp.exp(score - top)
        total = jnp.sum(e, axis=0, keepdims=True) + jnp.exp(sink - top)
        probs = (e * (1.0 / total)).astype(BF)
        wide = dot(v_cols, probs)
        return jnp.where(upper, wide[HEAD:, :], wide[:HEAD, :]).astype(BF)

    docs0 = column(doc_row[:, 0:128])
    docs1 = column(doc_row[:, 128:256])
    att[1, y, c] = attend(keys[...], vt[:, 128:384], jnp.concatenate([docs0, docs1], axis=0), 128)

    pl.semaphore_wait(barrier, TP - 1 + SP - 1)

    after = {"sp": lax.rem(sp + 1, SP)}
    send(keys.at[128:256], tail_k, tail_sem.at[0], tail_sem.at[3], after)
    send(values.at[128:256], tail_v, tail_sem.at[1], tail_sem.at[4], after)
    send(docs.at[:, 128:256], tail_d, tail_sem.at[2], tail_sem.at[5], after)

    def heads_go(block):
        for k in (4, 3, 5, 2, 6, 1, 7):
            send(att.at[block, y, c], att.at[block, y, c], a_send.at[block], a_recv.at[block], on_y(k))

    heads_go(1)

    for copy in in_copies[5:]:
        copy.wait()
    wot[...] = (jnp.transpose(out_weight[...].astype(F32)) * head_gain[...]).astype(BF)
    res[...] = ALPHA * jnp.transpose(residual[...].astype(F32))
    over = jnp.sum(wot[...].astype(F32), axis=0, keepdims=True)
    res_sum = jnp.sum(res[...], axis=0, keepdims=True)
    facts[y, c] = jnp.concatenate(
        [norm_gain[...], norm_shift[...], res_sum[:, 0:128], res_sum[:, 128:256]]
        + [over[:, 128 * i : 128 * i + 128] for i in range(8)],
        axis=0,
    )
    for k in (4, 3, 5, 2, 6, 1, 7):
        send(facts.at[y, c], facts.at[y, c], f_send.at[0], f_recv.at[0], on_y(k))

    arrived(tail_k, tail_sem.at[0], tail_sem.at[3], after)
    arrived(tail_v, tail_sem.at[1], tail_sem.at[4], after)
    arrived(tail_d, tail_sem.at[2], tail_sem.at[5], after)
    vt[:, 0:WINDOW] = jnp.transpose(tail_v[...].astype(F32)).astype(BF)
    before_docs = jnp.where(sp > 0, tail_d[...].astype(F32), -1.0)
    att[0, y, c] = attend(
        jnp.concatenate([tail_k[...], keys[0:128, :]], axis=0),
        vt[:, 0:256],
        jnp.concatenate([column(before_docs), docs0], axis=0),
        0,
    )

    heads_go(0)

    r0, r1 = routes[0:1, :], routes[1:2, :]
    experts = lax.broadcasted_iota(jnp.int32, (SP, TOK), 0)
    first_hit, second_hit = r0 == experts, r1 == experts
    named = jnp.where(first_hit | second_hit, 1.0, 0.0)
    earlier = jnp.where(
        lax.broadcasted_iota(jnp.int32, (TOK, TOK), 0) < lax.broadcasted_iota(jnp.int32, (TOK, TOK), 1), 1.0, 0.0
    ).astype(BF)
    place = jnp.where(named > 0.0, dot(named.astype(BF), earlier), -1.0)
    l0, l1 = logits[0:1, :], logits[1:2, :]
    l_top = jnp.maximum(l0, l1)
    e0, e1 = jnp.exp(l0 - l_top), jnp.exp(l1 - l_top)
    per = 1.0 / (e0 + e1)
    share = jnp.where(first_hit, e0 * per, jnp.where(second_hit, e1 * per, 0.0))
    slots = lax.broadcasted_iota(jnp.int32, (CAP, TOK), 0).astype(F32)
    for group in range(4):
        hits, weights = [], []
        for e in range(8 * group, 8 * group + 8):
            hit = place[e : e + 1, :] == slots
            hits.append(jnp.where(hit, 1.0, 0.0))
            weights.append(jnp.where(hit, share[e : e + 1, :], 0.0))
        rows = pl.ds(group * 8 * CAP, 8 * CAP)
        weight = jnp.concatenate(weights, axis=0)
        high = weight.astype(BF)
        select[rows, :] = jnp.concatenate(hits, axis=0).astype(BF)
        mix_hi[rows, :] = high
        mix_lo[rows, :] = (weight - high.astype(F32)).astype(BF)
    gain1, shift1 = twice(column(norm_gain[...])), twice(column(norm_shift[...]))

    arrived(facts.at[0:7, c], f_send.at[0], f_recv.at[0], on_y(1))
    send(facts.at[:, c], facts.at[:, c], f_send.at[1], f_recv.at[1], sibling)
    arrived(att.at[1, 0:7, c], a_send.at[1], a_recv.at[1], on_y(1))
    send(att.at[1, :, c], att.at[1, :, c], as_send.at[1], as_recv.at[1], sibling)
    arrived(facts.at[:, 1 - c], f_send.at[1], f_recv.at[1], sibling)

    fact = jnp.sum(facts[...].reshape(TP, 12, 128), axis=0) * (1.0 / D)
    over = jnp.concatenate([fact[4 + i : 5 + i] for i in range(8)], axis=1)
    over = jnp.broadcast_to(over, (8, TP * HEAD)).astype(BF)

    firsts, centred = [], []
    for block in (1, 0):
        if block == 0:
            arrived(att.at[0, 0:7, c], a_send.at[0], a_recv.at[0], on_y(1))
            send(att.at[0, :, c], att.at[0, :, c], as_send.at[0], as_recv.at[0], sibling)
        arrived(att.at[block, :, 1 - c], as_send.at[block], as_recv.at[block], sibling)
        heads = att[block].reshape(TP * HEAD, 128)
        wide = heads.astype(F32)
        scale = lax.rsqrt(jnp.sum(wide * wide, axis=0, keepdims=True) * (1.0 / (TP * HEAD)) + EPS)
        value = res[:, 128 * block : 128 * block + 128] + dot(wot[...], heads) * scale
        middle = fact[2 + block : 3 + block] + dot(over, heads)[0:1] * scale
        firsts.append(value)
        centred.append((value - middle).astype(BF))
    first = jnp.concatenate([firsts[1], firsts[0]], axis=1)
    centred = jnp.concatenate([centred[1], centred[0]], axis=1)
    hid[...] = first

    def tell(value, stat, send_sem, recv_sem):
        stat[tp] = jnp.concatenate(
            [jnp.sum(value, axis=0, keepdims=True), jnp.sum(value * value, axis=0, keepdims=True)], axis=0
        )

        def one(k, carry):
            send(stat.at[tp], stat.at[tp], send_sem, recv_sem, {"tp": lax.rem(tp + k, TP)})
            return carry

        lax.fori_loop(1, TP, one, 0)

    def hear(stat, send_sem, recv_sem):
        arrived(stat.at[0 : TP - 1], send_sem, recv_sem, sibling)
        total = jnp.sum(stat[...], axis=0)
        center = total[0:1] * (1.0 / D)
        spread = total[1:2] * (1.0 / D) - center * center
        return center, lax.rsqrt(spread + EPS)

    packed = dot_nt(select[...], centred)
    going[...] = packed.reshape(SP, CAP, COLS).astype(BF)
    own = pltpu.make_async_copy(going.at[sp], came.at[0], own_sem.at[0])
    own.start()
    for k in range(1, SP):
        to = lax.rem(z + 8 - PLACES[k][0], 8) * 4 + lax.rem(x + 4 - PLACES[k][1], 4)
        send(going.at[to], came.at[k], d_send.at[0], d_recv.at[k // 16], {"sp": to})
    tell(first, stat1, s_send.at[0], s_recv.at[0])

    w_copies[0].wait()
    w_copies[1].wait()

    def fold(i, carry):
        sums, shifts = carry
        at = pl.ds(pl.multiple_of(i * 128, 128), 128)
        fact = facts[lax.div(i, 2), lax.rem(i, 2)]
        gain_wide, shift_wide = column(fact[0:1]), column(fact[1:2])
        new_sums, new_shifts = [], []
        for j in range(6):
            lanes = slice(128 * j, 128 * j + 128)
            weight = wgu[at, lanes].astype(F32)
            gained = (weight * gain_wide).astype(BF)
            wgu[at, lanes] = gained
            new_sums.append(jnp.sum(gained.astype(F32), axis=0, keepdims=True))
            new_shifts.append(jnp.sum(weight * shift_wide, axis=0, keepdims=True))
        return sums + jnp.concatenate(new_sums, axis=1), shifts + jnp.concatenate(new_shifts, axis=1)

    none = jnp.zeros((1, 2 * FFB), F32)
    w_sums, w_shifts = lax.fori_loop(0, TP, fold, (none, none))
    rows_gu[0:1, :] = w_sums
    rows_gu[1:2, :] = w_shifts

    def piece(owner, quarter, core):
        return grid.at[chip(owner) * 2 + core, quarter]

    def ring_send(m, lanes):
        hops, quarter = lanes[m]
        if lanes is RIGHT:
            p = piece(NY - hops, quarter, c)
            send(p, p, gr_send.at[0], gr_recv.at[m], on_y(1))
        else:
            p = piece(hops, quarter, c)
            send(p, p, gl_send.at[0], gl_recv.at[m], on_y(NY - 1))

    def begin(half):
        block = came[16 * half : 16 * half + 16].astype(F32).reshape(HALF, COLS).astype(BF)
        grid[tp, 2 * half] = block[:QUARTER]
        grid[tp, 2 * half + 1] = block[QUARTER:]
        for m in (4 * half, 4 * half + 1):
            ring_send(m, RIGHT)
            ring_send(m, LEFT)
        p = grid.at[tp, 2 * half : 2 * half + 2]
        send(p, p, gs_send.at[0], gs_recv.at[half], sibling)

    def ring_take(m):
        for lanes in (RIGHT, LEFT):
            hops, quarter = lanes[m]
            right = lanes is RIGHT
            owner = NY - 1 - hops if right else hops + 1
            p = piece(owner, quarter, c)
            s, r = (gr_send, gr_recv) if right else (gl_send, gl_recv)
            arrived(p, s.at[0], r.at[m], on_y(1 if right else NY - 1))
            if (hops + 1, quarter) in lanes:
                ring_send(lanes.index((hops + 1, quarter)), lanes)
            send(p, p, gs_send.at[0], gs_recv.at[2 * owner + quarter // 2], sibling)

    def multiply(owner, half):
        at = chip(owner)
        rows = slice(2 * half, 2 * half + 2)
        arrived(grid.at[at * 2 + 1 - c, rows], gs_send.at[0], gs_recv.at[2 * owner + half], sibling)
        one, two = grid[at * 2, rows].reshape(HALF, COLS), grid[at * 2 + 1, rows].reshape(HALF, COLS)
        product = dot(jnp.concatenate([one, two], axis=1), wgu[pl.ds(pl.multiple_of(at * 256, 256), 256), :])
        one, two = one.astype(F32), two.astype(F32)
        if owner == 0:
            acc[half] = product
            acc1[half] = one + two
            acc2[half] = one * one + two * two
        else:
            acc[half] += product
            acc1[half] += one + two
            acc2[half] += one * one + two * two

    def activate(half):
        center = jnp.sum(acc1[half], axis=1, keepdims=True) * (1.0 / D)
        spread = jnp.sum(acc2[half], axis=1, keepdims=True) * (1.0 / D) - center * center
        scale = lax.rsqrt(spread + EPS)
        gate = (acc[half, :, 0:FFB] - center * rows_gu[0:1, 0:FFB]) * scale + rows_gu[1:2, 0:FFB]
        up = (acc[half, :, FFB:] - center * rows_gu[0:1, FFB:]) * scale + rows_gu[1:2, FFB:]
        mid[half] = (gate / (1.0 + jnp.exp(-gate)) * up).astype(BF)

    arrived(came.at[1:16], d_send.at[0], d_recv.at[0], after)
    own.wait()
    begin(0)
    multiply(0, 0)
    ring_take(0)
    ring_take(1)
    arrived(came.at[16:32], d_send.at[0], d_recv.at[1], after)
    begin(1)
    multiply(1, 0)
    multiply(7, 0)
    ring_take(2)
    multiply(0, 1)
    ring_take(3)
    center, scale = hear(stat1, s_send.at[0], s_recv.at[0])
    hid[...] = (hid[...] - center) * scale * gain1 + shift1
    ring_take(4)
    multiply(2, 0)
    ring_take(5)
    multiply(6, 0)
    ring_take(6)
    multiply(1, 1)
    ring_take(7)
    multiply(7, 1)
    ring_take(8)
    multiply(3, 0)
    ring_take(9)
    multiply(5, 0)
    ring_take(10)
    multiply(2, 1)
    ring_take(11)
    multiply(4, 0)
    activate(0)

    pltpu.make_async_copy(wd, wd, w_sem.at[2]).wait()
    waited = set()

    def partials(i, half):
        rows = slice(2 * half, 2 * half + 2)
        product = dot(mid[half], wd[chip(DESTS[i])])
        mine[i, rows] = product[:, 0:COLS].reshape(2, QUARTER, COLS)
        sib_out[i, rows] = product[:, COLS:].astype(BF).reshape(2, QUARTER, COLS)
        send(sib_out.at[i, rows], sib_in.at[i, rows], rs_send.at[0], rs_recv.at[2 * i + half], sibling)

    def summed(i, quarter):
        half = quarter // 2
        if (i, half) not in waited:
            waited.add((i, half))
            rows = slice(2 * half, 2 * half + 2)
            arrived(sib_in.at[i, rows], rs_send.at[0], rs_recv.at[2 * i + half], sibling)
        return mine[i, quarter] + sib_in[i, quarter].astype(F32)

    def passed(lanes, hops, quarter):
        m = lanes.index((hops, quarter))
        if lanes is SUM_RIGHT:
            arrived(right_in.at[m], rr_send.at[0], rr_recv.at[m], on_y(1))
            return right_in[m].astype(F32)
        arrived(left_in.at[m], rl_send.at[0], rl_recv.at[m], on_y(NY - 1))
        return left_in[m].astype(F32)

    def pass_on(m):
        for lanes in (SUM_RIGHT, SUM_LEFT):
            hops, quarter = lanes[m]
            right = lanes is SUM_RIGHT
            value = summed(DESTS.index(hops if right else NY - hops), quarter)
            if (hops + 1, quarter) in lanes:
                value = value + passed(lanes, hops + 1, quarter)
            if right:
                right_out[m] = value.astype(BF)
                send(right_out.at[m], right_in.at[m], rr_send.at[0], rr_recv.at[m], on_y(1))
            else:
                left_out[m] = value.astype(BF)
                send(left_out.at[m], left_in.at[m], rl_send.at[0], rl_recv.at[m], on_y(NY - 1))

    partials(0, 0)
    partials(1, 0)
    partials(2, 0)
    ring_take(12)
    multiply(6, 1)
    pass_on(0)
    pass_on(1)
    multiply(3, 1)
    multiply(5, 1)
    ring_take(13)
    multiply(4, 1)
    activate(1)
    partials(0, 1)
    partials(1, 1)
    partials(2, 1)
    pass_on(2)
    pass_on(3)
    pass_on(4)
    partials(3, 0)
    partials(4, 0)
    partials(3, 1)
    partials(4, 1)
    pass_on(5)
    pass_on(6)
    partials(5, 0)
    partials(6, 0)
    pass_on(7)
    pass_on(8)
    partials(5, 1)
    partials(6, 1)
    pass_on(9)
    partials(7, 1)
    partials(7, 0)
    pass_on(10)
    pass_on(11)
    pass_on(12)
    pass_on(13)

    def back_go(half):
        values = [
            summed(7, q) + passed(SUM_RIGHT, 1, q) + passed(SUM_LEFT, 1, q) for q in (2 * half, 2 * half + 1)
        ]
        value = jnp.concatenate(values, axis=0)
        back_out[16 * half : 16 * half + 16] = value.reshape(16, CAP, COLS).astype(BF)
        for k in range(max(1, 16 * half), 16 * half + 16):
            to = lax.rem(z + PLACES[k][0], 8) * 4 + lax.rem(x + PLACES[k][1], 4)
            send(back_out.at[k], back_in.at[sp], b_send.at[0], b_recv.at[0], {"sp": to})

    back_go(1)
    back_go(0)
    own2 = pltpu.make_async_copy(back_out.at[0], back_in.at[sp], own_sem.at[1])
    own2.start()
    gain2, shift2 = twice(column(final_gain[...])), twice(column(final_shift[...]))
    arrived(back_in.at[0 : SP - 1], b_send.at[0], b_recv.at[0], after)
    own2.wait()

    returned = jnp.transpose(back_in[...].astype(F32).reshape(ROWS, COLS)).astype(BF)
    moe = dot(returned, mix_hi[...]) + dot(returned, mix_lo[...])
    second = ALPHA * hid[...] + moe
    tell(second, stat2, s_send.at[1], s_recv.at[1])
    center, scale = hear(stat2, s_send.at[1], s_recv.at[1])
    out[...] = jnp.transpose((second - center) * scale * gain2 + shift2).astype(BF)

    for i in range(3):
        left_here((tail_k, tail_v, tail_d)[i], tail_sem.at[i], tail_sem.at[3 + i], after)
    for block in range(2):
        left_here(att.at[block, 0:7, 0], a_send.at[block], a_recv.at[block], on_y(1))
        left_here(att.at[block, :, 0], as_send.at[block], as_recv.at[block], sibling)
        left_here(stat1.at[0 : TP - 1], s_send.at[block], s_recv.at[block], sibling)
    left_here(facts.at[0:7, 0], f_send.at[0], f_recv.at[0], on_y(1))
    left_here(facts.at[:, 0], f_send.at[1], f_recv.at[1], sibling)
    left_here(going.at[0 : SP - 1], d_send.at[0], d_recv.at[0], after)
    left_here(back_out.at[0 : SP - 1], b_send.at[0], b_recv.at[0], after)
    left_here(right_out, gr_send.at[0], gr_recv.at[0], on_y(1))
    left_here(left_out, gl_send.at[0], gl_recv.at[0], on_y(NY - 1))
    left_here(right_out, rr_send.at[0], rr_recv.at[0], on_y(1))
    left_here(left_out, rl_send.at[0], rl_recv.at[0], on_y(NY - 1))
    left_here(sib_out, gs_send.at[0], gs_recv.at[0], sibling)
    left_here(sib_out, rs_send.at[0], rs_recv.at[0], sibling)


def local(
    residual, queries, keys, values, documents, sinks, head_gain, out_weight, norm_gain, norm_shift,
    routes, route_logits, gate_weight, up_weight, down_weight, final_gain, final_shift,
):
    vmem = pl.BlockSpec(memory_space=pltpu.VMEM)
    hbm = pl.BlockSpec(memory_space=pl.ANY)
    dma = pltpu.SemaphoreType.DMA
    return pl.pallas_call(
        kernel,
        out_shape=pltpu.VMEM((TOK, COLS), BF),
        in_specs=[hbm] * 17,
        out_specs=vmem,
        scratch_shapes=[
            pltpu.VMEM((TOK, COLS), BF),
            pltpu.VMEM((HEAD, TOK), BF),
            pltpu.VMEM((TOK, 128), BF),
            pltpu.VMEM((TOK, 128), BF),
            pltpu.VMEM((1, TOK), jnp.int32),
            pltpu.VMEM((1, 1), F32),
            pltpu.VMEM((1, TP * HEAD), F32),
            pltpu.VMEM((TP * HEAD, COLS), BF),
            pltpu.VMEM((1, COLS), F32),
            pltpu.VMEM((1, COLS), F32),
            pltpu.VMEM((2, TOK), jnp.int32),
            pltpu.VMEM((2, TOK), F32),
            pltpu.VMEM((1, COLS), F32),
            pltpu.VMEM((1, COLS), F32),
            pltpu.VMEM((D, 2 * FFB), BF),
            pltpu.VMEM((NY, FFB, 2 * COLS), BF),
            pltpu.VMEM((WINDOW, 128), BF),
            pltpu.VMEM((WINDOW, 128), BF),
            pltpu.VMEM((1, WINDOW), jnp.int32),
            pltpu.VMEM((COLS, TP * HEAD), BF),
            pltpu.VMEM((COLS, TOK), F32),
            pltpu.VMEM((128, WINDOW + TOK), BF),
            pltpu.VMEM((ROWS, TOK), BF),
            pltpu.VMEM((ROWS, TOK), BF),
            pltpu.VMEM((ROWS, TOK), BF),
            pltpu.VMEM((NY, 2, 12, 128), F32),
            pltpu.VMEM((2, 2 * FFB), F32),
            pltpu.VMEM((2, NY, 2, HEAD, 128), BF),
            pltpu.VMEM((TP, 2, TOK), F32),
            pltpu.VMEM((TP, 2, TOK), F32),
            pltpu.VMEM((COLS, TOK), F32),
            pltpu.VMEM((SP, CAP, COLS), BF),
            pltpu.VMEM((SP, CAP, COLS), BF),
            pltpu.VMEM((TP, 4, QUARTER, COLS), BF),
            pltpu.VMEM((2, HALF, 2 * FFB), F32),
            pltpu.VMEM((2, HALF, COLS), F32),
            pltpu.VMEM((2, HALF, COLS), F32),
            pltpu.VMEM((2, HALF, FFB), BF),
            pltpu.VMEM((NY, 4, QUARTER, COLS), F32),
            pltpu.VMEM((NY, 4, QUARTER, COLS), BF),
            pltpu.VMEM((NY, 4, QUARTER, COLS), BF),
            pltpu.VMEM((MESSAGES, QUARTER, COLS), BF),
            pltpu.VMEM((MESSAGES, QUARTER, COLS), BF),
            pltpu.VMEM((MESSAGES, QUARTER, COLS), BF),
            pltpu.VMEM((MESSAGES, QUARTER, COLS), BF),
            pltpu.VMEM((SP, CAP, COLS), BF),
            pltpu.VMEM((SP, CAP, COLS), BF),
            dma((14,)), dma((3,)), dma((6,)),
            dma((2,)), dma((2,)), dma((2,)), dma((2,)), dma((2,)), dma((2,)), dma((2,)), dma((2,)),
            dma((1,)), dma((2,)),
            dma((1,)), dma((MESSAGES,)), dma((1,)), dma((MESSAGES,)), dma((1,)), dma((2 * NY,)),
            dma((1,)), dma((2 * NY,)), dma((1,)), dma((MESSAGES,)), dma((1,)), dma((MESSAGES,)),
            dma((1,)), dma((1,)), dma((2,)),
        ],
        compiler_params=pltpu.CompilerParams(
            collective_id=0, has_side_effects=True, vmem_limit_bytes=60 * 1024 * 1024
        ),
        name="layer",
    )(
        residual, queries.T, keys, values, documents.reshape(1, TOK), sinks.reshape(1, 1),
        head_gain.reshape(1, TP * HEAD), out_weight, norm_gain.reshape(1, COLS), norm_shift.reshape(1, COLS),
        routes.T, route_logits.T, final_gain.reshape(1, COLS), final_shift.reshape(1, COLS),
        gate_weight, up_weight, down_weight,
    )


def solution(mesh):
    return jax.shard_map(
        local,
        mesh=mesh,
        in_specs=(
            P("sp", "tp"), P("sp", "tp"), P("sp", None), P("sp", None), P("sp"), P("tp"), P(), P(None, "tp"),
            P("tp"), P("tp"), P("sp", None), P("sp", None), P("sp", None, "tp"), P("sp", None, "tp"),
            P("sp", "tp", None), P("tp"), P("tp"),
        ),
        out_specs=P("sp", "tp"),
        check_vma=False,
    )
```
